32 devices in a mesh: kv: 8 (over z, y), tp: 4 (over x, core).
Axes of the slice: x: 2, y: 2, z: 4, core: 2. Of those that a mesh axis runs over, the one named last changes fastest.
Arguments:
- tokens: bfloat16 [6144, 2048], P('kv'), may hold values from -6 to 6
- w_query: bfloat16 [2048, 4096], P(None, 'tp'), may hold values from -3.1819805 to 3.1819805
- w_latent: bfloat16 [2048, 256], replicated, may hold values from -0.13258252 to 0.13258252
- latent_gain: float32 [256], replicated, may hold values from 0.1 to 1.9
- w_output: bfloat16 [4096, 2048], P('tp'), may hold values from -2 to 2
- chosen: int32 [96, 32], P('kv'), may hold values from -1 to 95, as said below
Outputs:
- attended: bfloat16 [6144, 2048], P(('kv', 'tp'))
- log_total: float32 [6144, 16], P('kv', 'tp')
The draws below stay inside these ranges and needn't reach their ends.
Inputs may be any that keep to these rules, and one draw needn't show every extreme that they name: `chosen`: row g names blocks at or before block g, no block twice; entry 0 is g itself; entries -1 name nothing and stand after the others. The 12 rows of one device together name exactly 2 distinct blocks of every earlier device's positions and none of a later device's.
All inputs are finite; a program needn't handle non-finite values.
Results may differ from the reference program's by a relative error of at most 0.01.
Values may be sent and summed in bfloat16 or wider, within the bound.
A program may use at most 192 MiB of HBM per device.

```python
import math
import jax
import jax.numpy as jnp
from jax import lax

D = 2048
HEADS = 16
R = 256
BLK = 64
NSEL = 32
CAP = 2
TOK_DEV = 768
SEQ = 6144
N_TP = 4


def latent_base(key):
    return jax.random.truncated_normal(jax.random.fold_in(key, 7), -6.0, 6.0, (D, R), jnp.float32) * D ** (-0.5)


def draw_w_latent(key, part):
    return latent_base(key).astype(jnp.bfloat16)


def draw_w_query(key, part):
    drawn = jax.random.truncated_normal(jax.random.fold_in(key, 11), -6.0, 6.0, (D, HEADS, R), jnp.float32) * D ** (-0.5)
    return drawn.reshape(D, HEADS * R).astype(jnp.bfloat16)


def draw_chosen(key, part):
    per_device = TOK_DEV // BLK
    block_count = SEQ // BLK
    devices = SEQ // TOK_DEV
    key_offer = jax.random.fold_in(key, 21)
    key_popular = jax.random.fold_in(key, 22)
    key_noise = jax.random.fold_in(key, 23)
    offer_raw = jax.random.randint(key_offer, (devices, devices, per_device), 0, 1 << 16)
    offer_score = offer_raw * per_device + jnp.arange(per_device, dtype=jnp.int32)
    offer_rank = jnp.argsort(jnp.argsort(-offer_score, axis=2), axis=2)
    offered = offer_rank < CAP
    popular = jax.random.randint(key_popular, (devices,), 0, 4)
    blocks = jnp.arange(block_count, dtype=jnp.int32)
    owner = blocks // per_device
    local_part = blocks % per_device
    dev_row = owner[:, None]
    own_col = owner[None, :]
    local_row = local_part[:, None]
    is_offered = offered[dev_row, own_col, local_part[None, :]]
    rank_here = offer_rank[dev_row, own_col, local_part[None, :]]
    earlier = blocks[None, :] <= blocks[:, None]
    other_ok = (own_col < dev_row) & is_offered
    allowed = (own_col == dev_row) & earlier | other_ok
    forced = other_ok & ((own_col * CAP + rank_here) % per_device == local_row)
    hot = (own_col == 0) | (own_col == dev_row - 1) | (own_col == dev_row - devices // 2)
    bias = jnp.where(blocks[None, :] == blocks[:, None], 40, jnp.where(forced, 30, jnp.where(own_col == dev_row, 8, jnp.where(hot, 20, 2 * popular[own_col]))))
    noise = jax.random.randint(key_noise, (block_count, block_count), 0, 4096)
    score = (bias * 4096 + noise) * block_count + blocks[None, :]
    score = jnp.where(allowed, score, -1 - blocks[None, :])
    values, picked = lax.top_k(score, NSEL)
    return jnp.where(values >= 0, picked, -1).astype(jnp.int32)


def steps_of(stream_key, shape, split, smallest, high):
    def one(dim, blocks):
        steps = jax.random.uniform(jax.random.fold_in(jax.random.fold_in(stream_key, 6), dim), (blocks,), jnp.float32, smallest / len(split), high / len(split))
        return jnp.repeat(jnp.exp(steps), shape[dim] // blocks).reshape((-1,) + (1,) * (len(shape) - dim - 1))

    gain = one(*split[0])
    for cut in split[1:]:
        gain = gain * one(*cut)
    return gain


def normal_values(key, shape, scale, most, shards=(), kind=jnp.bfloat16):
    values = scale * jax.random.normal(key, shape, jnp.float32)
    if shards:
        values = values * steps_of(key, shape, shards, -0.22, 0.18)
    return jnp.clip(values, -most, most).astype(kind)


def setup_inputs(seed: int = 0) -> dict:
    key_of = jax.random.split(jax.random.key(seed), 7)
    tokens = normal_values(key_of[0], (SEQ, D), 1.0, 6.0, ((0, 8),))
    w_query = draw_w_query(jax.random.fold_in(key_of[6], 71), 0)
    w_latent = draw_w_latent(jax.random.fold_in(key_of[6], 71), 0)
    latent_gain = jnp.clip(1.0 + 0.18 * jax.random.normal(key_of[3], (R,), jnp.float32), 0.1, 1.9)
    w_output = normal_values(key_of[4], (HEADS * R, D), 8 ** -0.5, 2.0, ((0, 4),))
    chosen = draw_chosen(jax.random.fold_in(key_of[6], 71), 0)
    return {"tokens": tokens, "w_query": w_query, "w_latent": w_latent, "latent_gain": latent_gain, "w_output": w_output, "chosen": chosen}


epsilon = 1e-06

def latents_of(tokens, w_latent, latent_gain):
    projected = jnp.dot(tokens, w_latent, preferred_element_type=jnp.float32)
    inv_rms = lax.rsqrt(lax.optimization_barrier(jnp.mean(projected * projected, axis=-1, keepdims=True)) + epsilon)
    return (projected * inv_rms * latent_gain).astype(jnp.bfloat16)

def attend(query_part, key_rows, picked, query_blocks, blk_len, score_scale):
    group_size, picks_each = picked.shape
    offsets = jnp.arange(blk_len, dtype=jnp.int32)
    key_pos = (picked[:, :, None] * blk_len + offsets[None, None, :]).reshape(group_size, picks_each * blk_len)
    usable = jnp.repeat(picked >= 0, blk_len, axis=1)
    query_pos = query_blocks[:, None] * blk_len + offsets[None, :]
    allowed = usable[:, None, :] & (key_pos[:, None, :] <= query_pos[:, :, None])
    scores = jnp.einsum('gqhr,gkr->ghqk', query_part.astype(jnp.float32), key_rows.astype(jnp.float32)) * score_scale
    scores = jnp.where(allowed[:, None, :, :], scores, -jnp.inf)
    peak_score = lax.optimization_barrier(jnp.max(scores, axis=3, keepdims=True))
    raised = jnp.exp(scores - peak_score)
    total_mass = lax.optimization_barrier(jnp.sum(raised, axis=3))
    weights = raised.astype(jnp.bfloat16)
    summed = jnp.einsum('ghqk,gkr->gqhr', weights.astype(jnp.float32), key_rows.astype(jnp.float32))
    mass_t = jnp.transpose(total_mass, (0, 2, 1))
    heads_out = (summed / mass_t[..., None]).astype(jnp.bfloat16)
    log_part = jnp.transpose(peak_score[..., 0], (0, 2, 1)) + jnp.log(mass_t)
    return (heads_out, log_part)

def reference(tokens, w_query, w_latent, latent_gain, w_output, chosen):
    seq_len, width = tokens.shape
    lat_rank = w_latent.shape[1]
    head_count = w_query.shape[1] // lat_rank
    block_count, picks_each = chosen.shape
    blk_len = seq_len // block_count
    latent = latents_of(tokens, w_latent, latent_gain)
    queries = jnp.dot(tokens, w_query, preferred_element_type=jnp.float32).astype(jnp.bfloat16)
    queries = queries.reshape(block_count, blk_len, head_count, lat_rank)
    key_table = latent.reshape(block_count, blk_len, lat_rank)
    group_size = math.gcd(block_count, 8)
    score_scale = lat_rank ** (-0.5)

    def one_group(offset):
        picked = lax.dynamic_slice_in_dim(chosen, offset, group_size, 0)
        query_part = lax.dynamic_slice_in_dim(queries, offset, group_size, 0)
        key_rows = jnp.take(key_table, jnp.maximum(picked, 0), axis=0).reshape(group_size, picks_each * blk_len, lat_rank)
        query_blocks = offset + jnp.arange(group_size, dtype=jnp.int32)
        return attend(query_part, key_rows, picked, query_blocks, blk_len, score_scale)
    group_starts = jnp.arange(0, block_count, group_size, dtype=jnp.int32)
    heads_out, log_total = lax.map(one_group, group_starts)
    heads_flat = heads_out.reshape(seq_len, head_count * lat_rank)
    log_total = log_total.reshape(seq_len, head_count)
    group_cols = head_count // N_TP * lat_rank
    attended = jnp.zeros((seq_len, width), jnp.float32)
    for group_index in range(N_TP):
        low = group_index * group_cols
        partial_value = jnp.dot(heads_flat[:, low:low + group_cols], w_output[low:low + group_cols], preferred_element_type=jnp.float32)
        attended = attended + lax.optimization_barrier(partial_value.astype(jnp.bfloat16)).astype(jnp.float32)
    return (attended.astype(jnp.bfloat16), log_total)
```

```python
import functools

import jax
import jax.numpy as jnp
from jax import lax
from jax.experimental import pallas as pl
from jax.experimental.pallas import tpu as pltpu
from jax.sharding import PartitionSpec as P

CAP = 2
PAIR = 2
FAR = 1 << 30
LOG2E = 1.4426950408889634

epsilon = 1e-06


def latents_of(tokens, w_latent, latent_gain):
    projected = jnp.dot(tokens, w_latent, preferred_element_type=jnp.float32)
    inv_rms = lax.rsqrt(jnp.mean(projected * projected, axis=-1, keepdims=True) + epsilon)
    return (projected * inv_rms * latent_gain).astype(jnp.bfloat16)


def slot_table(hit_mask):
    counted = jnp.cumsum(hit_mask.astype(jnp.int32), axis=1) - 1
    slot_ids = jnp.arange(CAP, dtype=jnp.int32)
    match_mask = hit_mask[:, None, :] & (counted[:, None, :] == slot_ids[None, :, None])
    places = jnp.arange(hit_mask.shape[1], dtype=jnp.int32)
    found = jnp.sum(jnp.where(match_mask, places[None, None, :], 0), axis=2)
    return jnp.where(jnp.any(match_mask, axis=2), found, -1)


def attend_kernel(
    n_tp, blk, heads, rank, per_shard,
    q_ref, key_ref, pos_ref, w_ref, out_ref, log_ref,
    heads_buf, own, a_send, a_recv, x_send, x_recv, a_ss, a_rs, x_ss, x_rs,
):
    me = lax.axis_index("tp")
    pair, core = me // PAIR, me % PAIR
    groups = n_tp // PAIR
    partner = pair * PAIR + (PAIR - 1 - core)
    steps = groups * per_shard
    scale = rank ** (-0.5)
    factor = scale * LOG2E

    barrier = pltpu.get_barrier_semaphore()
    pl.semaphore_signal(barrier, inc=1, device_id={"tp": partner})
    for o in range(1, groups):
        pl.semaphore_signal(
            barrier, inc=1, device_id={"tp": lax.rem(pair + o, groups) * PAIR + core}
        )
    pl.semaphore_wait(barrier, groups)

    def near(s):
        return pltpu.make_async_remote_copy(
            src_ref=a_send.at[s], dst_ref=a_recv.at[s],
            send_sem=a_ss.at[s], recv_sem=a_rs.at[s], device_id={"tp": partner},
        )

    def cross(s):
        peer = lax.rem(pair + 1 + s // per_shard, groups) * PAIR + core
        return pltpu.make_async_remote_copy(
            src_ref=x_send.at[s], dst_ref=x_recv.at[s],
            send_sem=x_ss.at[s], recv_sem=x_rs.at[s], device_id={"tp": peer},
        )

    def attend(g, half):
        row0 = pl.multiple_of(g * blk, blk)
        q = jnp.concatenate(
            [q_ref[pl.ds(row0, blk), h * rank:(h + 1) * rank] for h in range(heads)], axis=0
        )
        keys = key_ref[...]
        s = lax.dot_general(q, keys, (((1,), (1,)), ((), ())), preferred_element_type=jnp.float32)
        pos = pos_ref[pl.ds(g, 1), :]
        query_pos = g * blk + lax.rem(
            lax.broadcasted_iota(jnp.int32, (heads * blk, 1), 0), jnp.int32(blk)
        )
        s = jnp.where(pos <= query_pos, s, -jnp.inf)
        peak = jnp.max(s, axis=1, keepdims=True)
        p = jnp.exp2((s - peak) * factor)
        mass = jnp.sum(p, axis=1, keepdims=True)
        summed = jnp.dot(p.astype(jnp.bfloat16), keys, preferred_element_type=jnp.float32)
        result = (summed / mass).astype(jnp.bfloat16)
        logs = peak * scale + jnp.log(mass)
        for h in range(heads):
            heads_buf[half * blk:(half + 1) * blk, h * rank:(h + 1) * rank] = (
                result[h * blk:(h + 1) * blk]
            )
        log_ref[pl.ds(row0, blk), :] = jnp.concatenate(
            [logs[h * blk:(h + 1) * blk] for h in range(heads)], axis=1
        )

    def finish(s):
        near(s).wait_recv()
        total = own[s] + a_recv[s].astype(jnp.float32)

        @pl.when(s < steps - per_shard)
        def _():
            x_send[s] = total.astype(jnp.bfloat16)
            cross(s).start()

        @pl.when(s >= steps - per_shard)
        def _():
            own[s] = total

    def step(s, carry):
        group = lax.rem(pair + 1 + s // per_shard, groups)
        inner = lax.rem(s, per_shard)
        attend((group * PAIR + (PAIR - 1 - core)) * per_shard + inner, 0)
        attend((group * PAIR + core) * per_shard + inner, 1)
        part = jnp.dot(heads_buf[...], w_ref[...], preferred_element_type=jnp.float32)
        a_send[s] = part[:blk].astype(jnp.bfloat16)
        own[s] = part[blk:]
        near(s).start()

        @pl.when(s >= 1)
        def _():
            finish(s - 1)

        return carry

    lax.fori_loop(0, steps, step, 0)
    finish(steps - 1)
    for i in range(per_shard):
        total = own[steps - per_shard + i]
        for o in range(groups - 1):
            slot = o * per_shard + i
            cross(slot).wait_recv()
            total = total + x_recv[slot].astype(jnp.float32)
        out_ref[i * blk:(i + 1) * blk, :] = total.astype(jnp.bfloat16)
    for s in range(steps):
        near(s).wait_send()
    for s in range(steps - per_shard):
        cross(s).wait_send()


def attend_and_reduce(queries, keys, positions, w_output, blk, rank):
    rows, width = queries.shape[0], w_output.shape[1]
    heads = queries.shape[1] // rank
    n_tp = lax.axis_size("tp")
    per_shard = rows // (n_tp * blk)
    steps = (n_tp // PAIR) * per_shard
    crossing = steps - per_shard
    return pl.pallas_call(
        functools.partial(attend_kernel, n_tp, blk, heads, rank, per_shard),
        out_shape=(
            jax.ShapeDtypeStruct((rows // n_tp, width), jnp.bfloat16),
            jax.ShapeDtypeStruct((rows, heads), jnp.float32),
        ),
        in_specs=[pl.BlockSpec(memory_space=pltpu.VMEM)] * 4,
        out_specs=[pl.BlockSpec(memory_space=pltpu.VMEM)] * 2,
        scratch_shapes=[
            pltpu.VMEM((PAIR * blk, heads * rank), jnp.bfloat16),
            pltpu.VMEM((steps, blk, width), jnp.float32),
            pltpu.VMEM((steps, blk, width), jnp.bfloat16),
            pltpu.VMEM((steps, blk, width), jnp.bfloat16),
            pltpu.VMEM((crossing, blk, width), jnp.bfloat16),
            pltpu.VMEM((crossing, blk, width), jnp.bfloat16),
            pltpu.SemaphoreType.DMA((steps,)),
            pltpu.SemaphoreType.DMA((steps,)),
            pltpu.SemaphoreType.DMA((crossing,)),
            pltpu.SemaphoreType.DMA((crossing,)),
        ],
        compiler_params=pltpu.CompilerParams(
            collective_id=0, has_side_effects=True, vmem_limit_bytes=56 * 1024 * 1024
        ),
    )(queries, keys, positions, w_output)


def local(tokens, w_query, w_latent, latent_gain, w_output, chosen):
    tok_rows = tokens.shape[0]
    lat_rank = w_latent.shape[1]
    per_device, picks_each = chosen.shape
    blk_len = tok_rows // per_device
    devices = lax.axis_size("kv")
    my_index = lax.axis_index("kv")
    every_block = jnp.arange(devices * per_device, dtype=jnp.int32)
    owners = jnp.arange(devices, dtype=jnp.int32)
    named = jnp.any(chosen[:, :, None] == every_block[None, None, :], axis=1)
    wanted = jnp.any(named, axis=0).reshape(devices, per_device)
    request = slot_table(wanted & (owners != my_index)[:, None])
    asked = lax.all_to_all(request, "kv", split_axis=0, concat_axis=0, tiled=True)
    latent = latents_of(tokens, w_latent, latent_gain)
    own_blocks = latent.reshape(per_device, blk_len, lat_rank)
    reply_blocks = jnp.take(own_blocks, jnp.maximum(asked, 0), axis=0)
    fetched = lax.all_to_all(reply_blocks, "kv", split_axis=0, concat_axis=0, tiled=True)
    keys = jnp.concatenate(
        [latent, fetched.reshape(devices * CAP * blk_len, lat_rank)], axis=0
    )
    queries = jnp.dot(tokens, w_query, preferred_element_type=jnp.float32).astype(jnp.bfloat16)

    own_ids = my_index * per_device + jnp.arange(per_device, dtype=jnp.int32)
    far_ids = jnp.where(request >= 0, owners[:, None] * per_device + request, -2).reshape(-1)
    slot_ids = jnp.concatenate([own_ids, far_ids])
    slot_named = jnp.any(chosen[:, :, None] == slot_ids[None, None, :], axis=1)
    key_named = jnp.repeat(slot_named, blk_len, axis=1)
    key_place = jnp.concatenate(
        [
            jnp.arange(tok_rows, dtype=jnp.int32),
            jnp.full((devices * CAP * blk_len,), -1, jnp.int32),
        ]
    )
    positions = jnp.where(key_named, key_place[None, :], FAR)
    return attend_and_reduce(queries, keys, positions, w_output, blk_len, lat_rank)


def solution(mesh):
    placed = (P("kv", None), P(None, "tp"), P(), P(), P("tp", None), P("kv", None))
    return jax.shard_map(
        local,
        mesh=mesh,
        in_specs=placed,
        out_specs=(P(("kv", "tp"), None), P("kv", "tp")),
        check_vma=False,
    )
```

```python
import functools

import jax
import jax.numpy as jnp
from jax import lax
from jax.experimental import pallas as pl
from jax.experimental.pallas import tpu as pltpu
from jax.sharding import PartitionSpec as P

CAP = 2
PAIR = 2
FAR = 1 << 30
LOG2E = 1.4426950408889634

epsilon = 1e-06


def fused_kernel(
    n_kv, n_tp, blk, heads, rank, per_device, picks, per_shard,
    tok_hbm, wq_hbm, wl_hbm, gain_ref, wo_hbm, chosen_ref, out_ref, log_ref,
    tok, wq, wl, wo, queries, keys, pos_ref, log_buf, req_send, asked, reply,
    heads_buf, own, a_send, a_recv, x_send, x_recv,
    load_sem, req_ss, req_rs, far_ss, far_rs, fwd_ss, fwd_rs, a_ss, a_rs, x_ss, x_rs,
):
    my = lax.axis_index("kv")
    me = lax.axis_index("tp")
    pair, core = me // PAIR, me % PAIR
    groups = n_tp // PAIR
    partner = pair * PAIR + (PAIR - 1 - core)
    steps = groups * per_shard
    scale = rank ** (-0.5)
    factor = scale * LOG2E
    rows = per_device * blk
    half_rows = blk // PAIR
    piece = CAP * half_rows
    chunk = rows // n_tp

    loads = [
        pltpu.make_async_copy(src, dst, load_sem.at[i])
        for i, (src, dst) in enumerate(
            [(tok_hbm, tok), (wl_hbm, wl), (wq_hbm, wq), (wo_hbm, wo)]
        )
    ]
    for load in loads:
        load.start()

    barrier = pltpu.get_barrier_semaphore()

    def greet(o, carry):
        pl.semaphore_signal(barrier, inc=1, device_id={"kv": lax.rem(my + o, n_kv)})
        return carry

    lax.fori_loop(1, n_kv, greet, 0)
    pl.semaphore_signal(barrier, inc=1, device_id={"tp": partner})
    for o in range(1, groups):
        pl.semaphore_signal(
            barrier, inc=1, device_id={"tp": lax.rem(pair + o, groups) * PAIR + core}
        )

    def ask(d, slot):
        return pltpu.make_async_remote_copy(
            src_ref=req_send.at[d], dst_ref=asked.at[slot],
            send_sem=req_ss.at[d], recv_sem=req_rs.at[slot], device_id={"kv": d},
        )

    def far_rows(d, side):
        return pl.ds(pl.multiple_of(rows + (d * PAIR + side) * piece, piece), piece)

    def answer(p, d):
        return pltpu.make_async_remote_copy(
            src_ref=reply.at[p], dst_ref=keys.at[far_rows(d, core)],
            send_sem=far_ss.at[p], recv_sem=far_rs.at[d], device_id={"kv": p},
        )

    def forward(d, side):
        return pltpu.make_async_remote_copy(
            src_ref=keys.at[far_rows(d, side)], dst_ref=keys.at[far_rows(d, side)],
            send_sem=fwd_ss.at[d], recv_sem=fwd_rs.at[d], device_id={"tp": partner},
        )

    lanes = pos_blocks(n_kv * per_device)
    block_ids = lax.broadcasted_iota(jnp.int32, (per_device, lanes), 1)
    named = jnp.zeros((per_device, lanes), jnp.int32)
    for j in range(picks):
        named = jnp.maximum(named, (chosen_ref[:, j:j + 1] == block_ids).astype(jnp.int32))
    wanted = jnp.broadcast_to(jnp.max(named, axis=0, keepdims=True), (8, lanes))
    named = named.astype(jnp.float32).astype(jnp.bfloat16)
    first = lax.broadcasted_iota(jnp.int32, (lanes, lanes), 0)
    second = lax.broadcasted_iota(jnp.int32, (lanes, lanes), 1)
    ahead = (first < second) & (first // per_device == second // per_device)
    counted = jnp.dot(
        wanted.astype(jnp.float32).astype(jnp.bfloat16),
        ahead.astype(jnp.float32).astype(jnp.bfloat16),
        preferred_element_type=jnp.float32,
    ).astype(jnp.int32)
    lane_block = lax.broadcasted_iota(jnp.int32, (8, lanes), 1)
    lane_owner = lane_block // per_device
    slot_of = jnp.where((wanted > 0) & (lane_owner < my), lane_owner * CAP + counted, -1)
    slot_of = jnp.where(counted < CAP, slot_of, -1)
    lane_local = lane_block - lane_owner * per_device

    slot3 = (
        lax.broadcasted_iota(jnp.int32, (n_kv, 8, lanes), 0) * CAP
        + lax.broadcasted_iota(jnp.int32, (n_kv, 8, lanes), 1)
    )
    real3 = lax.broadcasted_iota(jnp.int32, (n_kv, 8, lanes), 1) < CAP
    index3 = jnp.sum(
        jnp.where(real3 & (slot3 == slot_of[None]), lane_local[None], 0), axis=2, keepdims=True
    )
    req_send[...] = jnp.broadcast_to(index3, (n_kv, 8, 128))

    pl.semaphore_wait(barrier, n_kv - 1 + groups)

    def send_ask(d, carry):
        @pl.when(d < my)
        def _():
            ask(d, my).start()

        return carry

    lax.fori_loop(0, n_kv - 1, send_ask, 0)

    own_key = lax.broadcasted_iota(jnp.int32, (lanes, rows), 1)
    own_pick = (lax.broadcasted_iota(jnp.int32, (lanes, rows), 0) - my * per_device) == own_key // blk
    own_named = jnp.dot(
        named, own_pick.astype(jnp.float32).astype(jnp.bfloat16), preferred_element_type=jnp.float32
    )
    place = lax.broadcasted_iota(jnp.int32, (per_device, rows), 1)
    pos_ref[:, :rows] = jnp.where(own_named > 0.5, place, FAR)
    slots = n_kv * CAP
    match = (
        jnp.broadcast_to(slot_of[:1], (slots, lanes))
        == lax.broadcasted_iota(jnp.int32, (slots, lanes), 0)
    )
    slot_named = lax.dot_general(
        named, match.astype(jnp.float32).astype(jnp.bfloat16), (((1,), (1,)), ((), ())),
        preferred_element_type=jnp.float32,
    )
    far_count = (n_kv - 1) * CAP * blk
    far_key = lax.broadcasted_iota(jnp.int32, (slots, far_count), 1)
    key_slot = far_key // (CAP * blk) * CAP + far_key // half_rows % CAP
    spread = key_slot == lax.broadcasted_iota(jnp.int32, (slots, far_count), 0)
    far_named = jnp.dot(
        slot_named.astype(jnp.bfloat16), spread.astype(jnp.float32).astype(jnp.bfloat16),
        preferred_element_type=jnp.float32,
    )
    pos_ref[:, rows:] = jnp.where(far_named > 0.5, -1, FAR)

    loads[0].wait()
    loads[1].wait()

    def latent_rows(i, carry):
        span = pl.ds(pl.multiple_of(i * chunk, chunk), chunk)
        projected = jnp.dot(tok[span, :], wl[...], preferred_element_type=jnp.float32)
        inv_rms = lax.rsqrt(jnp.mean(projected * projected, axis=-1, keepdims=True) + epsilon)
        keys[span, :] = (projected * inv_rms * gain_ref[...]).astype(jnp.bfloat16)
        return carry

    lax.fori_loop(0, n_tp, latent_rows, 0)

    def send_reply(o, carry):
        p = my + (n_kv - o)

        @pl.when(p < n_kv)
        def _():
            ask(my, p).wait_recv()
            want = asked[p]
            within = core * half_rows + lax.broadcasted_iota(jnp.int32, (half_rows, 1), 0)
            source = jnp.concatenate(
                [want[c:c + 1, :1] * blk + within for c in range(CAP)], axis=0
            )
            pick = lax.broadcasted_iota(jnp.int32, (piece, rows), 1) == source
            reply[p] = jnp.dot(
                pick.astype(jnp.float32).astype(jnp.bfloat16), keys[:rows, :],
                preferred_element_type=jnp.float32,
            ).astype(jnp.bfloat16)
            answer(p, my).start()

        return carry

    lax.fori_loop(1, n_kv, send_reply, 0)
    loads[2].wait()

    def query_rows(i, carry):
        span = pl.ds(pl.multiple_of(i * chunk, chunk), chunk)
        queries[span, :] = jnp.dot(
            tok[span, :], wq[...], preferred_element_type=jnp.float32
        ).astype(jnp.bfloat16)
        return carry

    def pass_on(d, carry):
        @pl.when(d < my)
        def _():
            answer(my, d).wait_recv()
            forward(d, core).start()

        @pl.when(d >= my)
        def _():
            whole = pl.ds(pl.multiple_of(rows + d * CAP * blk, CAP * blk), CAP * blk)
            keys[whole, :] = jnp.zeros((CAP * blk, rank), jnp.bfloat16)

        return carry

    def take_passed(d, carry):
        @pl.when(d < my)
        def _():
            forward(d, PAIR - 1 - core).wait_recv()

        return carry

    lax.fori_loop(0, n_tp - 1, query_rows, 0)
    lax.fori_loop(0, n_kv - 1, pass_on, 0)
    query_rows(n_tp - 1, 0)
    lax.fori_loop(0, n_kv - 1, take_passed, 0)
    loads[3].wait()

    def near(s):
        return pltpu.make_async_remote_copy(
            src_ref=a_send.at[s], dst_ref=a_recv.at[s],
            send_sem=a_ss.at[s], recv_sem=a_rs.at[s], device_id={"tp": partner},
        )

    def cross(s):
        peer = lax.rem(pair + 1 + s // per_shard, groups) * PAIR + core
        return pltpu.make_async_remote_copy(
            src_ref=x_send.at[s], dst_ref=x_recv.at[s],
            send_sem=x_ss.at[s], recv_sem=x_rs.at[s], device_id={"tp": peer},
        )

    def attend(g, half):
        row0 = pl.multiple_of(g * blk, blk)
        q = jnp.concatenate(
            [queries[pl.ds(row0, blk), h * rank:(h + 1) * rank] for h in range(heads)], axis=0
        )
        table = keys[...]
        s = lax.dot_general(q, table, (((1,), (1,)), ((), ())), preferred_element_type=jnp.float32)
        pos = pos_ref[pl.ds(g, 1), :]
        query_pos = g * blk + lax.rem(
            lax.broadcasted_iota(jnp.int32, (heads * blk, 1), 0), jnp.int32(blk)
        )
        s = jnp.where(pos <= query_pos, s, -jnp.inf)
        peak = jnp.max(s, axis=1, keepdims=True)
        p = jnp.exp2((s - peak) * factor)
        mass = jnp.sum(p, axis=1, keepdims=True)
        summed = jnp.dot(p.astype(jnp.bfloat16), table, preferred_element_type=jnp.float32)
        result = (summed / mass).astype(jnp.bfloat16)
        logs = peak * scale + jnp.log(mass)
        for h in range(heads):
            heads_buf[half * blk:(half + 1) * blk, h * rank:(h + 1) * rank] = (
                result[h * blk:(h + 1) * blk]
            )
        log_buf[pl.ds(row0, blk), :] = jnp.concatenate(
            [logs[h * blk:(h + 1) * blk] for h in range(heads)]
            + [jnp.zeros((blk, 128 - heads), jnp.float32)],
            axis=1,
        )

    def finish(s):
        near(s).wait_recv()
        total = own[s] + a_recv[s].astype(jnp.float32)

        @pl.when(s < steps - per_shard)
        def _():
            x_send[s] = total.astype(jnp.bfloat16)
            cross(s).start()

        @pl.when(s >= steps - per_shard)
        def _():
            own[s] = total

    def step(s, carry):
        group = lax.rem(pair + 1 + s // per_shard, groups)
        inner = lax.rem(s, per_shard)
        attend((group * PAIR + (PAIR - 1 - core)) * per_shard + inner, 0)
        attend((group * PAIR + core) * per_shard + inner, 1)
        part = jnp.dot(heads_buf[...], wo[...], preferred_element_type=jnp.float32)
        a_send[s] = part[:blk].astype(jnp.bfloat16)
        own[s] = part[blk:]
        near(s).start()

        @pl.when(s >= 1)
        def _():
            finish(s - 1)

        return carry

    lax.fori_loop(0, steps, step, 0)
    finish(steps - 1)
    for i in range(per_shard):
        total = own[steps - per_shard + i]
        for o in range(groups - 1):
            slot = o * per_shard + i
            cross(slot).wait_recv()
            total = total + x_recv[slot].astype(jnp.float32)
        out_ref[i * blk:(i + 1) * blk, :] = total.astype(jnp.bfloat16)
    for s in range(steps):
        near(s).wait_send()
    for s in range(steps - per_shard):
        cross(s).wait_send()
    log_ref[...] = log_buf[...].T[:heads]

    def drain(d, carry):
        @pl.when(d < my)
        def _():
            ask(d, my).wait_send()
            forward(d, core).wait_send()

        @pl.when(d + 1 > my)
        def _():
            answer(d + 1, my).wait_send()

        return carry

    lax.fori_loop(0, n_kv - 1, drain, 0)


def pos_blocks(count):
    return -(-count // 128) * 128


def local(tokens, w_query, w_latent, latent_gain, w_output, chosen):
    rows, width = tokens.shape[0], w_output.shape[1]
    rank = w_latent.shape[1]
    heads = w_query.shape[1] // rank
    per_device, picks = chosen.shape
    blk = rows // per_device
    n_kv, n_tp = lax.axis_size("kv"), lax.axis_size("tp")
    per_shard = per_device // n_tp
    steps = (n_tp // PAIR) * per_shard
    crossing = steps - per_shard
    n_keys = rows + (n_kv - 1) * CAP * blk
    piece = CAP * (blk // PAIR)
    any_spec = pl.BlockSpec(memory_space=pl.ANY)
    vmem_spec = pl.BlockSpec(memory_space=pltpu.VMEM)
    attended, log_rows = pl.pallas_call(
        functools.partial(
            fused_kernel, n_kv, n_tp, blk, heads, rank, per_device, picks, per_shard
        ),
        out_shape=(
            jax.ShapeDtypeStruct((rows // n_tp, width), jnp.bfloat16),
            jax.ShapeDtypeStruct((heads, rows), jnp.float32),
        ),
        in_specs=[any_spec, any_spec, any_spec, vmem_spec, any_spec, vmem_spec],
        out_specs=[vmem_spec, vmem_spec],
        scratch_shapes=[
            pltpu.VMEM(tokens.shape, jnp.bfloat16),
            pltpu.VMEM(w_query.shape, jnp.bfloat16),
            pltpu.VMEM(w_latent.shape, jnp.bfloat16),
            pltpu.VMEM(w_output.shape, jnp.bfloat16),
            pltpu.VMEM((rows, heads * rank), jnp.bfloat16),
            pltpu.VMEM((n_keys, rank), jnp.bfloat16),
            pltpu.VMEM((per_device, n_keys), jnp.int32),
            pltpu.VMEM((rows, 128), jnp.float32),
            pltpu.VMEM((n_kv, 8, 128), jnp.int32),
            pltpu.VMEM((n_kv, 8, 128), jnp.int32),
            pltpu.VMEM((n_kv, piece, rank), jnp.bfloat16),
            pltpu.VMEM((PAIR * blk, heads * rank), jnp.bfloat16),
            pltpu.VMEM((steps, blk, width), jnp.float32),
            pltpu.VMEM((steps, blk, width), jnp.bfloat16),
            pltpu.VMEM((steps, blk, width), jnp.bfloat16),
            pltpu.VMEM((crossing, blk, width), jnp.bfloat16),
            pltpu.VMEM((crossing, blk, width), jnp.bfloat16),
            pltpu.SemaphoreType.DMA((4,)),
        ]
        + [pltpu.SemaphoreType.DMA((n_kv,))] * 6
        + [pltpu.SemaphoreType.DMA((steps,))] * 2
        + [pltpu.SemaphoreType.DMA((crossing,))] * 2,
        compiler_params=pltpu.CompilerParams(
            collective_id=0, has_side_effects=True, vmem_limit_bytes=60 * 1024 * 1024
        ),
    )(tokens, w_query, w_latent, latent_gain[None, :], w_output, chosen)
    return attended, log_rows.T


def solution(mesh):
    placed = (P("kv", None), P(None, "tp"), P(), P(), P("tp", None), P("kv", None))
    return jax.shard_map(
        local,
        mesh=mesh,
        in_specs=placed,
        out_specs=(P(("kv", "tp"), None), P("kv", "tp")),
        check_vma=False,
    )
```
